256 devices in a mesh: sp: 64 (over z, y, core), tp: 4 (over x).
Axes of the slice: x: 4, y: 4, z: 8, core: 2. Of those that a mesh axis runs over, the one named last changes fastest.
Arguments:
- stream: bfloat16 [65536, 4096], P('sp', 'tp'), may hold values from -11 to 11
- norm_gain: bfloat16 [3, 4096], P(None, 'tp'), may hold values from 0.099609375 to 1.8984375
- pool_weight: bfloat16 [3, 4, 1024, 1024], P(None, 'tp', 'sp'), may hold values from -0.1875 to 0.1875
- pool_scale: bfloat16 [3, 4096], P(None, 'tp'), may hold values from 0.099609375 to 1.8984375
Outputs:
- mixed: bfloat16 [65536, 4096], P('sp', 'tp')
The draws below stay inside these ranges and needn't reach their ends.
All inputs are finite; a program needn't handle non-finite values.
Results may differ from the reference program's by a relative error of at most 0.015.
Values may be sent and summed in bfloat16 or wider, within the bound.
No kernel may reach another device: no remote copies, remote signals or barrier semaphores. Data moves between devices by JAX's collectives and lax.ppermute only.
A program may use at most 64 MiB of HBM per device.

```python
import jax
import jax.numpy as jnp
from jax import lax

D = 4096
POOL_GROUPS = 4
LAYERS = 3
GC = 1024
TOKENS = 65536


def draw_stream(key, part):
    noise_key, perm_key, row_key = jax.random.split(key, 3)
    levels = 0.5 * 3.0 ** (jnp.arange(POOL_GROUPS, dtype=jnp.float32) / (POOL_GROUPS - 1))
    levels = jax.random.permutation(perm_key, levels)
    column_scale = jnp.repeat(levels, GC)
    base_vals = jax.random.truncated_normal(noise_key, -6.0, 6.0, (TOKENS, D), jnp.float32)
    return (base_vals * column_scale[None, :]).astype(jnp.bfloat16)


def shard_levels(key, extent, cuts, low, largest):
    gain = 1.0
    for dim, shards_of in cuts:
        draws = jax.random.uniform(jax.random.fold_in(jax.random.fold_in(key, 6), dim), (shards_of,), jnp.float32, low / len(cuts), largest / len(cuts))
        gain = gain * jnp.repeat(jnp.exp(draws), extent[dim] // shards_of).reshape((-1,) + (1,) * (len(extent) - 1 - dim))
    return gain


def noise(key, shape, scale, bound, cuts=(), kind=jnp.bfloat16):
    factor_of = shard_levels(key, shape, cuts, -0.22, 0.18) if cuts else 1.0
    drawn = jax.random.normal(key, shape, jnp.float32) * scale * factor_of
    return jnp.minimum(jnp.maximum(drawn, -bound), bound).astype(kind)


def setup_inputs(seed: int = 0) -> dict:
    splits = jax.random.split(jax.random.key(seed), 5)
    stream = draw_stream(jax.random.fold_in(splits[4], 71), 0)
    norm_gain = jnp.clip(1.0 + 0.18 * jax.random.normal(splits[1], (LAYERS, D), jnp.float32), 0.099609375, 1.8984375).astype(jnp.bfloat16)
    pool_weight = noise(splits[2], (LAYERS, POOL_GROUPS, GC, GC), GC ** -0.5, 0.1875, ((1, 4), (2, 64)))
    pool_scale = jnp.clip(1.0 + 0.18 * jax.random.normal(splits[3], (LAYERS, D), jnp.float32), 0.099609375, 1.8984375).astype(jnp.bfloat16)
    return {"stream": stream, "norm_gain": norm_gain, "pool_weight": pool_weight, "pool_scale": pool_scale}


norm_eps = 1e-06

def centred_mean(values, half_width):
    length = values.shape[0]
    sums = jnp.concatenate([jnp.zeros((1, values.shape[1]), jnp.float32), jnp.cumsum(values, axis=0)], axis=0)
    positions = jnp.arange(length)
    low_end = jnp.maximum(positions - half_width, 0)
    high_end = jnp.minimum(positions + half_width, length)
    return (sums[high_end] - sums[low_end]) / (high_end - low_end).astype(jnp.float32)[:, None]

def reference(stream, norm_gain, pool_weight, pool_scale):
    current = stream
    for layer_idx in range(LAYERS):
        stream_f = current.astype(jnp.float32)
        meansq = lax.optimization_barrier(jnp.mean(stream_f * stream_f, axis=1, keepdims=True))
        normed = (stream_f * lax.rsqrt(meansq + norm_eps) * norm_gain[layer_idx].astype(jnp.float32)).astype(jnp.bfloat16)
        pieces = []
        for group in range(POOL_GROUPS):
            members = normed[:, group * GC:(group + 1) * GC].astype(jnp.float32)
            pooled = (centred_mean(members, 2 ** group) - members).astype(jnp.bfloat16)
            pieces.append(jnp.dot(pooled, pool_weight[layer_idx, group], preferred_element_type=jnp.float32))
        branch = jnp.concatenate(pieces, axis=1)
        current = (stream_f + branch * pool_scale[layer_idx].astype(jnp.float32)).astype(jnp.bfloat16)
    return current
```

```python
import functools

import jax
import jax.numpy as jnp
from jax import lax
from jax.experimental import pallas as pl
from jax.experimental.pallas import tpu as pltpu
from jax.sharding import PartitionSpec as P

D = 4096
EPS = 1e-06
HALO = 32
Z, Y, C = 8, 4, 2
VMEM = pl.BlockSpec(memory_space=pltpu.VMEM)


def split(sp):
    return sp // (Y * C), (sp // C) % Y, sp % C


def join(z, y, c):
    return ((z % Z) * Y + y % Y) * C + c


def pairs(dz, dy, swap=False):
    found = []
    for sp in range(Z * Y * C):
        z, y, c = split(sp)
        sign = 1 if c == 0 else -1
        found.append((sp, join(z + sign * dz, y + sign * dy, 1 - c if swap else c)))
    return found


def ring_z(value):
    return lax.ppermute(value, "sp", pairs(1, 0))


def ring_y(value):
    return lax.ppermute(value, "sp", pairs(0, 1))


def partner(value):
    return lax.ppermute(value, "sp", pairs(0, 0, True))


def line_y(c):
    def half(c):
        s = 2 * c - 1
        return [(0, c), (s, c), (s, 1 - c), (2, c)]
    return half(c) + half(1 - c)


def line_z(c):
    def half(c):
        s = 2 * c - 1
        out = [(0, c)]
        for k in (1, 2, 3):
            out += [(s * k, c), (s * k, 1 - c)]
        return out + [(4, c)]
    return half(c) + half(1 - c)


def gather(weight):
    own = weight
    chip = jnp.stack([own, partner(own)])
    half = weight.shape[-1] // 2
    a, b = chip[..., :half], chip[..., half:]
    a1 = ring_y(a)
    b1 = ring_z(b)
    a2 = ring_y(a1[:1])
    b2 = ring_z(b1)
    mine = jnp.concatenate([a[:1], a1, a2])
    la = jnp.concatenate([mine, a[1:], partner(mine[1:])])
    b3 = ring_z(b2)
    f1 = ring_z(la)
    b4 = ring_z(b3[:1])
    mine = jnp.concatenate([b[:1], b1, b2, b3, b4])
    lb = jnp.concatenate([mine, b[1:], partner(mine[1:])])
    f2 = ring_z(f1)
    g1 = ring_y(lb)
    f3 = ring_z(f2)
    f4 = ring_z(f3[:4])
    g2 = ring_y(g1[:8])

    def s(c):
        return 2 * c - 1

    left = [(la, lambda c: [(0, y, k) for y, k in line_y(c)])]
    for k, f in ((1, f1), (2, f2), (3, f3), (4, f4)):
        n = f.shape[0]
        left.append((f, lambda c, k=k, n=n: [(s(c) * k, y, q) for y, q in line_y(c)[:n]]))
        left.append((partner(f), lambda c, k=k, n=n: [(s(1 - c) * k, y, q) for y, q in line_y(1 - c)[:n]]))
    right = [(lb, lambda c: [(z, 0, k) for z, k in line_z(c)])]
    for k, g in ((1, g1), (2, g2)):
        n = g.shape[0]
        right.append((g, lambda c, k=k, n=n: [(z, s(c) * k, q) for z, q in line_z(c)[:n]]))
        right.append((partner(g), lambda c, k=k, n=n: [(z, s(1 - c) * k, q) for z, q in line_z(1 - c)[:n]]))
    return left, right


def squares(x):
    rows = x.shape[0]
    lane = lax.broadcasted_iota(jnp.int32, (128, 128), 1)
    cols = jnp.zeros((128, 128), jnp.float32)
    for i in range(0, rows, 128):
        n = min(128, rows - i)
        part = x[i : i + n]
        if n < 128:
            part = jnp.concatenate([part, jnp.zeros((128 - n, part.shape[1]), jnp.float32)])
        cols = jnp.where(lane == i // 128, jnp.sum(part, axis=1, keepdims=True), cols)
    return cols.T[:16]


def first_kernel(before, x, after, ext, sums):
    rows = x.shape[0]
    ext[:HALO] = before[...]
    ext[HALO : HALO + rows] = x[...]
    ext[HALO + rows :] = after[...]
    total = ext.shape[0]
    acc = jnp.zeros((total, 128), jnp.float32)
    for j in range(0, x.shape[1], 128):
        v = ext[:, j : j + 128].astype(jnp.float32)
        acc += v * v
    sums[...] = squares(acc)


def layer_kernel(layer, lo, hi, last, owners, n_left, tokens, *refs):
    n = len(owners)
    x_ref, gain_ref, scale_ref, s0, s1, s2, s3 = refs[:7]
    pieces = refs[7 : 7 + n]
    out_ref = refs[7 + n]
    rest = refs[8 + n :]
    if last:
        normed, pooled, w, acc = rest
    else:
        sums_ref, normed, pooled, w, acc = rest
    total, width = x_ref.shape
    sp = lax.axis_index("sp")
    z, y, c = sp // (Y * C), lax.rem(sp // C, Y), lax.rem(sp, C)

    for i, (ref, owner) in enumerate(zip(pieces, owners, strict=True)):
        cols = pl.ds(0, width // 2) if i < n_left else pl.ds(width // 2, width // 2)
        for j, ((z0, y0, c0), (z1, y1, c1)) in enumerate(zip(owner(0), owner(1), strict=True)):
            dz, dy = jnp.where(c == 0, z0, z1), jnp.where(c == 0, y0, y1)
            core = jnp.where(c == 0, c0, c1)
            at = (lax.rem(z + dz + Z, Z) * Y + lax.rem(y + dy + Y, Y)) * C + core
            w[pl.ds(pl.multiple_of(at * 16, 16), 16), cols] = ref[j, layer]

    scale_of = lax.rsqrt((s0[...] + s1[...] + s2[...] + s3[...]) / D + EPS)
    column = jnp.concatenate([scale_of, jnp.zeros((112, 128), jnp.float32)]).T
    gain = gain_ref[layer : layer + 1, :].astype(jnp.float32)
    for i in range(0, total, 128):
        m = min(128, total - i)
        r = column[:m, i // 128 : i // 128 + 1]
        normed[i : i + m] = (x_ref[i : i + m].astype(jnp.float32) * r * gain).astype(jnp.bfloat16)

    first = sp * (total - 2 * HALO) - HALO
    half = jnp.left_shift(jnp.int32(1), lax.axis_index("tp"))
    step = 224
    for b in range(lo, hi, step):
        m = min(step, hi - b)
        k = m + 32
        t = first + b + lax.broadcasted_iota(jnp.int32, (m, k), 0)
        s = first + b - 16 + lax.broadcasted_iota(jnp.int32, (m, k), 1)
        inside = (s >= jnp.maximum(t - half, 0)) & (s < jnp.minimum(t + half, tokens))
        count = jnp.maximum(jnp.minimum(t + half, tokens) - jnp.maximum(t - half, 0), 1)
        band = jnp.where(inside, 1.0 / count.astype(jnp.float32), 0.0) - (s == t).astype(jnp.float32)
        pooled[b - lo : b - lo + m] = jnp.dot(
            band.astype(jnp.bfloat16), normed[b - 16 : b - 16 + k], preferred_element_type=jnp.float32
        ).astype(jnp.bfloat16)

    scale = scale_ref[layer : layer + 1, :].astype(jnp.float32)
    rows = hi - lo
    mstep = 352 if rows % 352 == 0 else 256
    if not last:
        acc[...] = jnp.zeros_like(acc)
        out_ref[:lo] = x_ref[:lo]
        out_ref[hi:] = x_ref[hi:]
    for j in range(0, width, 256):
        for i in range(0, rows, mstep):
            branch = jnp.dot(
                pooled[i : i + mstep], w[:, j : j + 256], preferred_element_type=jnp.float32
            )
            new = x_ref[lo + i : lo + i + mstep, j : j + 256].astype(jnp.float32) + branch * scale[:, j : j + 256]
            new = new.astype(jnp.bfloat16)
            if last:
                out_ref[i : i + mstep, j : j + 256] = new
            else:
                out_ref[lo + i : lo + i + mstep, j : j + 256] = new
                new = new.astype(jnp.float32)
                new = new * new
                acc[lo + i : lo + i + mstep] += new[:, :128] + new[:, 128:]
    if not last:
        sums_ref[...] = squares(acc[...])


def over_tp(sums):
    n = lax.axis_size("tp")
    return [sums] + [lax.ppermute(sums, "tp", [(i, (i + k) % n) for i in range(n)]) for k in (1, n - 1, 2)]


def local(stream, norm_gain, pool_weight, pool_scale):
    rows, width = stream.shape
    layers, _, shard, _ = pool_weight.shape
    devices = lax.axis_size("sp")
    total = rows + 2 * HALO
    up = [(i, i + 1) for i in range(devices - 1)]
    before = lax.ppermute(stream[rows - HALO :], "sp", up)
    after = lax.ppermute(stream[:HALO], "sp", [(j, i) for i, j in up])
    left, right = gather(pool_weight.reshape(layers, shard, width))
    pieces = [p for p, _ in left + right]
    owners = [o for _, o in left + right]
    params = pltpu.CompilerParams(vmem_limit_bytes=32 * 2**20)
    sums_type = jax.ShapeDtypeStruct((16, 128), jnp.float32)
    ext_type = jax.ShapeDtypeStruct((total, width), jnp.bfloat16)
    ext, sums = pl.pallas_call(
        first_kernel,
        out_shape=(ext_type, sums_type),
        in_specs=[VMEM] * 3,
        out_specs=(VMEM, VMEM),
        compiler_params=params,
        name="first",
    )(before, stream, after)
    for layer in range(layers):
        last = layer == layers - 1
        lo, hi = (HALO, HALO + rows) if last else (16, total - 16)
        out = jax.ShapeDtypeStruct((rows, width), jnp.bfloat16) if last else (ext_type, sums_type)
        scratch = [
            pltpu.VMEM((total, width), jnp.bfloat16),
            pltpu.VMEM((hi - lo, width), jnp.bfloat16),
            pltpu.VMEM((width, width), jnp.bfloat16),
            pltpu.VMEM((total, 128), jnp.float32),
        ]
        out = pl.pallas_call(
            functools.partial(layer_kernel, layer, lo, hi, last, owners, len(left), rows * devices),
            out_shape=out,
            in_specs=[VMEM] * (7 + len(pieces)),
            out_specs=VMEM if last else (VMEM, VMEM),
            scratch_shapes=scratch,
            compiler_params=params,
            cost_estimate=pl.CostEstimate(
                flops=2 * total * width * width, bytes_accessed=4 * total * width, transcendentals=0
            ),
            name=f"layer{layer}",
        )(ext, norm_gain, pool_scale, *over_tp(sums), *pieces)
        if not last:
            ext, sums = out
    return out


def solution(mesh):
    placed = (P("sp", "tp"), P(None, "tp"), P(None, "tp", "sp", None), P(None, "tp"))
    return jax.shard_map(
        local, mesh=mesh, in_specs=placed, out_specs=P("sp", "tp"), check_vma=False
    )
```

```python
import functools

import jax
import jax.numpy as jnp
from jax import lax
from jax.experimental import pallas as pl
from jax.experimental.pallas import tpu as pltpu
from jax.sharding import PartitionSpec as P


D = 4096
EPS = 1e-06
HALO = 32
Z, Y, C = 8, 4, 2
VMEM = pl.BlockSpec(memory_space=pltpu.VMEM)


def split(sp):
    return sp // (Y * C), (sp // C) % Y, sp % C


def join(z, y, c):
    return ((z % Z) * Y + y % Y) * C + c


def toward(i, c):
    return 1 - 2 * ((i + c) % 2)


def trade(value, axis, step):
    found = []
    for sp in range(Z * Y * C):
        z, y, c = split(sp)
        sign = (2, 1, -1)[step]
        if axis == "z":
            to = join(z + sign * toward(z, c), y, c)
        else:
            to = join(z, y + sign * toward(y, c), c)
        found.append((sp, to))
    return lax.ppermute(value, "sp", found)


def partner(value):
    return lax.ppermute(value, "sp", [(sp, sp ^ 1) for sp in range(Z * Y * C)])


RING4 = (0, 1, -1, -2)
RING8 = (0, 1, -1, -2, 2, 3, -3, -4)


def after(value, other):
    return lax.optimization_barrier((value, other))[0]


def pack(parts, lo, hi):
    def kernel(*refs):
        out, at = refs[-1], 0
        for ref in refs[:-1]:
            n = ref.shape[0]
            out[at : at + n] = ref[:, lo:hi]
            at += n

    slots, _, *tail = parts[0].shape
    slots = sum(p.shape[0] for p in parts)
    return pl.pallas_call(
        kernel,
        out_shape=jax.ShapeDtypeStruct((slots, hi - lo, *tail), parts[0].dtype),
        in_specs=[VMEM] * len(parts),
        out_specs=VMEM,
        compiler_params=pltpu.CompilerParams(vmem_limit_bytes=2**23),
        name="pack",
    )(*parts)


def slots(zs, ys):
    return [(z, y) for z in zs for y in ys]


def gather(own, fetched):
    layers = own.shape[1]
    beside = [trade(own, "y", 1), trade(own, "y", 2), trade(own, "y", 0)]
    behind = trade(own, "z", 1)

    line = pack((fetched, *beside), 0, 1)
    near = pack((line, trade(line, "z", 1)), 0, 1)
    second = trade(near, "z", 2)
    third = trade(second, "z", 1)
    fourth = trade(third, "z", 2)
    here = slots(RING8[:4], RING4)
    inner = pack((near, second), 0, 1)
    early = partner(inner)
    outer = pack((third, fourth), 0, 1)
    there = slots(RING8[4:], RING4)
    out = [[(inner, here, 0), (early, here, 1), (outer, there, 0), (partner(outer), there, 1)]]

    two = pack((fetched, behind), 1, layers)
    second = trade(two, "z", 2)
    third = trade(second, "z", 1)
    line = pack((two, second, third, after(trade(third, "z", 2), early)), 0, layers - 1)
    beside = after(trade(line, "y", 1), fourth)
    for i in range(layers - 1):
        near = pack((line, beside), i, i + 1)
        far = trade(near, "y", 2)
        out.append((near, far))
    return out, early


def finish(near, far, other):
    piece = pack((near, after(far, other)), 0, 1)
    where = [(z, y) for y in RING4 for z in RING8]
    return [(piece, where, 0), (partner(piece), where, 1)]


def squares(x):
    rows = x.shape[0]
    lane = lax.broadcasted_iota(jnp.int32, (128, 128), 1)
    cols = jnp.zeros((128, 128), jnp.float32)
    for i in range(0, rows, 128):
        n = min(128, rows - i)
        part = x[i : i + n]
        if n < 128:
            part = jnp.concatenate([part, jnp.zeros((128 - n, part.shape[1]), jnp.float32)])
        cols = jnp.where(lane == i // 128, jnp.sum(part, axis=1, keepdims=True), cols)
    return cols.T[:16]


def prepare_kernel(own, x, kept, within, across, edge, arrived):
    rows = x.shape[0]
    copies = [
        pltpu.make_async_copy(x.at[pl.ds(0, HALO)], edge.at[0], arrived.at[0]),
        pltpu.make_async_copy(x.at[pl.ds(rows - HALO, HALO)], edge.at[1], arrived.at[1]),
        pltpu.make_async_copy(own, kept, arrived.at[2]),
    ]
    for copy in copies:
        copy.start()
    even = lax.rem(lax.axis_index("sp"), 2) == 0
    for copy in copies[:2]:
        copy.wait()
    within[...] = jnp.where(even, edge[1], edge[0])
    across[...] = jnp.where(even, edge[0], edge[1])
    copies[2].wait()


def add_kernel(a, b, out):
    out[...] = a[...] + b[...]


def first_kernel(within, across, x, ext, sums, arrived):
    rows = x.shape[0]
    total = ext.shape[0]
    part = rows // 4
    copies = [
        pltpu.make_async_copy(
            x.at[pl.ds(i * part, part)], ext.at[pl.ds(HALO + i * part, part)], arrived.at[i]
        )
        for i in range(4)
    ]
    for copy in copies:
        copy.start()
    even = lax.rem(lax.axis_index("sp"), 2) == 0
    ext[:HALO] = jnp.where(even, across[...], within[...])
    ext[HALO + rows :] = jnp.where(even, within[...], across[...])
    acc = []
    edges = (0, HALO + part, HALO + 2 * part, HALO + 3 * part, total)
    for i, (lo, hi) in enumerate(zip(edges, edges[1:])):
        copies[i].wait()
        found = jnp.zeros((hi - lo, 128), jnp.float32)
        for j in range(0, x.shape[1], 128):
            v = ext[lo:hi, j : j + 128].astype(jnp.float32)
            found += v * v
        acc.append(found)
    sums[...] = squares(jnp.concatenate(acc))


def map_kernel(layer, places, x_ref, gain_ref, *refs):
    pieces, (out_ref, w) = refs[: len(places)], refs[len(places) :]
    total, width = x_ref.shape
    sp = lax.axis_index("sp")
    z, y, c = sp // (Y * C), lax.rem(sp // C, Y), lax.rem(sp, C)

    for ref, (where, other) in zip(pieces, places, strict=True):
        core = 1 - c if other else c
        dz, dy = 1 - 2 * lax.rem(z + core, 2), 1 - 2 * lax.rem(y + core, 2)
        for j, (fz, fy) in enumerate(where):
            at = (lax.rem(z + fz * dz + Z, Z) * Y + lax.rem(y + fy * dy + Y, Y)) * C + core
            w[pl.ds(pl.multiple_of(at * 16, 16), 16), :] = ref[j, 0]

    gain = gain_ref[layer : layer + 1, :].astype(jnp.float32)
    step = 272
    for i in range(0, total, step):
        scaled = (x_ref[i : i + step].astype(jnp.float32) * gain).astype(jnp.bfloat16)
        for j in range(0, width, 256):
            out_ref[i : i + step, j : j + 256] = jnp.dot(
                scaled, w[:, j : j + 256], preferred_element_type=jnp.float32
            )


def pool_kernel(layer, lo, hi, last, tokens, n_parts, *refs):
    x_ref, mapped_ref, scale_ref, *refs = refs
    parts, refs = refs[:n_parts], refs[n_parts:]
    if last:
        out_ref, normed, held, sent = refs
    else:
        out_ref, sums_ref, normed, acc = refs
    total, width = x_ref.shape
    scale_of = lax.rsqrt(sum(p[...] for p in parts) / D + EPS)
    column = jnp.concatenate([scale_of, jnp.zeros((112, 128), jnp.float32)]).T
    for i in range(0, total, 128):
        m = min(128, total - i)
        r = column[:m, i // 128 : i // 128 + 1]
        normed[i : i + m] = (mapped_ref[i : i + m] * r).astype(jnp.bfloat16)

    first = lax.axis_index("sp") * (total - 2 * HALO) - HALO
    half = jnp.left_shift(jnp.int32(1), lax.axis_index("tp"))
    scale = scale_ref[layer : layer + 1, :].astype(jnp.float32)
    if not last:
        acc[:lo] = jnp.zeros((lo, 128), jnp.float32)
        acc[hi:] = jnp.zeros((total - hi, 128), jnp.float32)
        out_ref[:lo] = x_ref[:lo]
        out_ref[hi:] = x_ref[hi:]
    step = 224
    copies = []
    for b in range(lo, hi, step):
        m = min(step, hi - b)
        k = m + 32
        t = first + b + lax.broadcasted_iota(jnp.int32, (m, k), 0)
        s = first + b - 16 + lax.broadcasted_iota(jnp.int32, (m, k), 1)
        inside = (s >= jnp.maximum(t - half, 0)) & (s < jnp.minimum(t + half, tokens))
        count = jnp.maximum(jnp.minimum(t + half, tokens) - jnp.maximum(t - half, 0), 1)
        band = jnp.where(inside, 1.0 / count.astype(jnp.float32), 0.0) - (s == t).astype(jnp.float32)
        band = band.astype(jnp.bfloat16)
        squared = None
        for j in range(0, width, 256):
            branch = jnp.dot(band, normed[b - 16 : b - 16 + k, j : j + 256], preferred_element_type=jnp.float32)
            new = x_ref[b : b + m, j : j + 256].astype(jnp.float32) + branch * scale[:, j : j + 256]
            new = new.astype(jnp.bfloat16)
            if last:
                held[b - lo : b - lo + m, j : j + 256] = new
            else:
                out_ref[b : b + m, j : j + 256] = new
                new = new.astype(jnp.float32)
                new = new * new
                new = new[:, :128] + new[:, 128:]
                squared = new if squared is None else squared + new
        if last:
            rows = pl.ds(b - lo, m)
            copies.append(pltpu.make_async_copy(held.at[rows], out_ref.at[rows], sent.at[len(copies)]))
            copies[-1].start()
        else:
            acc[b : b + m] = squared
    if not last:
        sums_ref[...] = squares(acc[...])
    for copy in copies:
        copy.wait()


def over_tp(sums):
    n = lax.axis_size("tp")
    found = [sums]
    for k in (1, 3, 2):
        found.append(lax.ppermute(sums, "tp", [(i, i ^ k) for i in range(n)]))
    return found


def program(stream, norm_gain, pool_weight, pool_scale):
    rows, width = stream.shape
    layers, _, shard, _ = pool_weight.shape
    devices = lax.axis_size("sp")
    total = rows + 2 * HALO
    own = pool_weight.reshape(1, layers, shard, width)
    edge = jax.ShapeDtypeStruct((HALO, width), stream.dtype)
    fetched, within, across = pl.pallas_call(
        prepare_kernel,
        out_shape=(jax.ShapeDtypeStruct(own.shape, own.dtype), edge, edge),
        in_specs=[pl.BlockSpec(memory_space=pltpu.HBM)] * 2,
        out_specs=(VMEM,) * 3,
        scratch_shapes=[pltpu.VMEM((2, HALO, width), stream.dtype), pltpu.SemaphoreType.DMA((3,))],
        compiler_params=pltpu.CompilerParams(vmem_limit_bytes=125 * 2**19),
        name="prepare",
    )(own, stream)
    within = lax.ppermute(within, "sp", [(i, i ^ 1) for i in range(devices)])
    pairs = [(i, i + 1) for i in range(1, devices - 1, 2)]
    across = lax.ppermute(across, "sp", pairs + [(j, i) for i, j in pairs])
    params = pltpu.CompilerParams(vmem_limit_bytes=32 * 2**20)
    sums_type = jax.ShapeDtypeStruct((16, 128), jnp.float32)
    ext_type = jax.ShapeDtypeStruct((total, width), jnp.bfloat16)
    ext, sums = pl.pallas_call(
        first_kernel,
        out_shape=(ext_type, sums_type),
        in_specs=[VMEM, VMEM, pl.BlockSpec(memory_space=pltpu.HBM)],
        out_specs=(VMEM, VMEM),
        scratch_shapes=[pltpu.SemaphoreType.DMA((4,))],
        compiler_params=params,
        name="first",
    )(within, across, stream)
    other = lax.ppermute(sums, "tp", [(i, i ^ 1) for i in range(lax.axis_size("tp"))])
    gathered, early = gather(own, fetched)
    other = after(other, early)
    sums = pl.pallas_call(
        add_kernel, out_shape=sums_type, in_specs=[VMEM] * 2, out_specs=VMEM,
        compiler_params=pltpu.CompilerParams(vmem_limit_bytes=2**20), name="add",
    )(sums, other)
    other = lax.ppermute(sums, "tp", [(i, i ^ 3) for i in range(lax.axis_size("tp"))])
    traded = [sums, other]
    for layer in range(layers):
        pieces = finish(*gathered[layer], sums) if layer else gathered[0]
        last = layer == layers - 1
        lo, hi = (HALO, HALO + rows) if last else (16, total - 16)
        mapped = pl.pallas_call(
            functools.partial(map_kernel, layer, [p[1:] for p in pieces]),
            out_shape=jax.ShapeDtypeStruct((total, width), jnp.float32),
            in_specs=[VMEM] * (2 + len(pieces)),
            out_specs=VMEM,
            scratch_shapes=[pltpu.VMEM((width, width), jnp.bfloat16)],
            compiler_params=params,
            cost_estimate=pl.CostEstimate(
                flops=2 * total * width * width, bytes_accessed=6 * total * width, transcendentals=0
            ),
        )(ext, norm_gain, *[p[0] for p in pieces])
        scratch = [pltpu.VMEM((total, width), jnp.bfloat16)]
        if last:
            scratch += [pltpu.VMEM((rows, width), jnp.bfloat16), pltpu.SemaphoreType.DMA((5,))]
        else:
            scratch.append(pltpu.VMEM((total, 128), jnp.float32))
        out = pl.pallas_call(
            functools.partial(pool_kernel, layer, lo, hi, last, rows * devices, len(traded)),
            out_shape=jax.ShapeDtypeStruct((rows, width), jnp.bfloat16) if last else (ext_type, sums_type),
            in_specs=[VMEM] * (3 + len(traded)),
            out_specs=pl.BlockSpec(memory_space=pltpu.HBM) if last else (VMEM, VMEM),
            scratch_shapes=scratch,
            compiler_params=params,
            cost_estimate=pl.CostEstimate(
                flops=total * width * 512, bytes_accessed=8 * total * width, transcendentals=0
            ),
        )(ext, mapped, pool_scale, *traded)
        if not last:
            ext, sums = out
            traded = over_tp(sums)
    return out


def solution(mesh):
    placed = (P("sp", "tp"), P(None, "tp"), P(None, "tp", "sp", None), P(None, "tp"))
    return jax.shard_map(program, mesh=mesh, in_specs=placed, out_specs=P("sp", "tp"), check_vma=False)
```

```python
import functools

import jax
import jax.numpy as jnp
from jax import lax
from jax.experimental import pallas as pl
from jax.experimental.pallas import tpu as pltpu
from jax.sharding import PartitionSpec as P


D = 4096
EPS = 1e-06
HALO = 32
Z, Y, C = 8, 4, 2
VMEM = pl.BlockSpec(memory_space=pltpu.VMEM)


def split(sp):
    return sp // (Y * C), (sp // C) % Y, sp % C


def join(z, y, c):
    return ((z % Z) * Y + y % Y) * C + c


def toward(i, c):
    return 1 - 2 * ((i + c) % 2)


def trade(value, axis, step):
    found = []
    for sp in range(Z * Y * C):
        z, y, c = split(sp)
        sign = (2, 1, -1)[step]
        if axis == "z":
            to = join(z + sign * toward(z, c), y, c)
        else:
            to = join(z, y + sign * toward(y, c), c)
        found.append((sp, to))
    return lax.ppermute(value, "sp", found)


def partner(value):
    return lax.ppermute(value, "sp", [(sp, sp ^ 1) for sp in range(Z * Y * C)])


RING4 = (0, 1, -1, -2)
RING8 = (0, 1, -1, -2, 2, 3, -3, -4)


def after(value, other):
    return lax.optimization_barrier((value, other))[0]


def pack(parts, lo, hi):
    def kernel(*refs):
        out, at = refs[-1], 0
        for ref in refs[:-1]:
            n = ref.shape[0]
            out[at : at + n] = ref[:, lo:hi]
            at += n

    slots, _, *tail = parts[0].shape
    slots = sum(p.shape[0] for p in parts)
    return pl.pallas_call(
        kernel,
        out_shape=jax.ShapeDtypeStruct((slots, hi - lo, *tail), parts[0].dtype),
        in_specs=[VMEM] * len(parts),
        out_specs=VMEM,
        compiler_params=pltpu.CompilerParams(vmem_limit_bytes=2**23),
        name="pack",
    )(*parts)


def slots(zs, ys):
    return [(z, y) for z in zs for y in ys]


def gather(own, fetched):
    layers = own.shape[1]
    beside = [trade(own, "y", 1), trade(own, "y", 2), trade(own, "y", 0)]
    behind = trade(own, "z", 1)

    line = pack((fetched, *beside), 0, 1)
    near = pack((line, trade(line, "z", 1)), 0, 1)
    second = trade(near, "z", 2)
    third = trade(second, "z", 1)
    fourth = trade(third, "z", 2)
    here = slots(RING8[:4], RING4)
    inner = pack((near, second), 0, 1)
    early = partner(inner)
    outer = pack((third, fourth), 0, 1)
    there = slots(RING8[4:], RING4)
    out = [[(inner, here, 0), (early, here, 1), (outer, there, 0), (partner(outer), there, 1)]]

    two = pack((fetched, behind), 1, layers)
    second = trade(two, "z", 2)
    third = trade(second, "z", 1)
    line = pack((two, second, third, trade(third, "z", 2)), 0, layers - 1)
    beside = trade(line, "y", 1)
    for i in range(layers - 1):
        near = pack((line, beside), i, i + 1)
        far = trade(near, "y", 2)
        out.append((near, far))
    return out, early


def finish(near, far, other):
    piece = pack((near, after(far, other)), 0, 1)
    where = [(z, y) for y in RING4 for z in RING8]
    return [(piece, where, 0), (partner(piece), where, 1)]


def squares(x):
    rows = x.shape[0]
    lane = lax.broadcasted_iota(jnp.int32, (128, 128), 1)
    cols = jnp.zeros((128, 128), jnp.float32)
    for i in range(0, rows, 128):
        n = min(128, rows - i)
        part = x[i : i + n]
        if n < 128:
            part = jnp.concatenate([part, jnp.zeros((128 - n, part.shape[1]), jnp.float32)])
        cols = jnp.where(lane == i // 128, jnp.sum(part, axis=1, keepdims=True), cols)
    return cols.T[:16]


def prepare_kernel(own, x, kept, within, across, edge, arrived):
    rows = x.shape[0]
    copies = [
        pltpu.make_async_copy(x.at[pl.ds(0, HALO)], edge.at[0], arrived.at[0]),
        pltpu.make_async_copy(x.at[pl.ds(rows - HALO, HALO)], edge.at[1], arrived.at[1]),
        pltpu.make_async_copy(own, kept, arrived.at[2]),
    ]
    for copy in copies:
        copy.start()
    even = lax.rem(lax.axis_index("sp"), 2) == 0
    for copy in copies[:2]:
        copy.wait()
    within[...] = jnp.where(even, edge[1], edge[0])
    across[...] = jnp.where(even, edge[0], edge[1])
    copies[2].wait()


def add_kernel(a, b, out):
    out[...] = a[...] + b[...]


def first_kernel(within, across, x, ext, sums, arrived):
    rows = x.shape[0]
    total = ext.shape[0]
    part = rows // 4
    copies = [
        pltpu.make_async_copy(
            x.at[pl.ds(i * part, part)], ext.at[pl.ds(HALO + i * part, part)], arrived.at[i]
        )
        for i in range(4)
    ]
    for copy in copies:
        copy.start()
    even = lax.rem(lax.axis_index("sp"), 2) == 0
    ext[:HALO] = jnp.where(even, across[...], within[...])
    ext[HALO + rows :] = jnp.where(even, within[...], across[...])
    acc = []
    edges = (0, HALO + part, HALO + 2 * part, HALO + 3 * part, total)
    for i, (lo, hi) in enumerate(zip(edges, edges[1:])):
        copies[i].wait()
        found = jnp.zeros((hi - lo, 128), jnp.float32)
        for j in range(0, x.shape[1], 128):
            v = ext[lo:hi, j : j + 128].astype(jnp.float32)
            found += v * v
        acc.append(found)
    sums[...] = squares(jnp.concatenate(acc))


def map_kernel(layer, places, x_ref, gain_ref, *refs):
    pieces, (out_ref, w) = refs[: len(places)], refs[len(places) :]
    total, width = x_ref.shape
    sp = lax.axis_index("sp")
    z, y, c = sp // (Y * C), lax.rem(sp // C, Y), lax.rem(sp, C)

    for ref, (where, other) in zip(pieces, places, strict=True):
        core = 1 - c if other else c
        dz, dy = 1 - 2 * lax.rem(z + core, 2), 1 - 2 * lax.rem(y + core, 2)
        for j, (fz, fy) in enumerate(where):
            at = (lax.rem(z + fz * dz + Z, Z) * Y + lax.rem(y + fy * dy + Y, Y)) * C + core
            w[pl.ds(pl.multiple_of(at * 16, 16), 16), :] = ref[j, 0]

    gain = gain_ref[layer : layer + 1, :].astype(jnp.float32)
    step = 1088
    for i in range(0, total, step):
        scaled = (x_ref[i : i + step].astype(jnp.float32) * gain).astype(jnp.bfloat16)
        for j in range(0, width, 256):
            out_ref[i : i + step, j : j + 256] = jnp.dot(
                scaled, w[:, j : j + 256], preferred_element_type=jnp.float32
            )


def pool_kernel(layer, lo, hi, last, tokens, n_parts, *refs):
    x_ref, mapped_ref, scale_ref, *refs = refs
    parts, refs = refs[:n_parts], refs[n_parts:]
    if last:
        out_ref, normed, held, sent = refs
    else:
        out_ref, sums_ref, normed, acc = refs
    total, width = x_ref.shape
    scale_of = lax.rsqrt(sum(p[...] for p in parts) / D + EPS)
    column = jnp.concatenate([scale_of, jnp.zeros((112, 128), jnp.float32)]).T
    for i in range(0, total, 128):
        m = min(128, total - i)
        r = column[:m, i // 128 : i // 128 + 1]
        normed[i : i + m] = (mapped_ref[i : i + m] * r).astype(jnp.bfloat16)

    first = lax.axis_index("sp") * (total - 2 * HALO) - HALO
    half = jnp.left_shift(jnp.int32(1), lax.axis_index("tp"))
    scale = scale_ref[layer : layer + 1, :].astype(jnp.float32)
    if not last:
        acc[:lo] = jnp.zeros((lo, 128), jnp.float32)
        acc[hi:] = jnp.zeros((total - hi, 128), jnp.float32)
        out_ref[:lo] = x_ref[:lo]
        out_ref[hi:] = x_ref[hi:]
    step = 224
    copies = []
    for b in range(lo, hi, step):
        m = min(step, hi - b)
        k = m + 32
        t = first + b + lax.broadcasted_iota(jnp.int32, (m, k), 0)
        s = first + b - 16 + lax.broadcasted_iota(jnp.int32, (m, k), 1)
        inside = (s >= jnp.maximum(t - half, 0)) & (s < jnp.minimum(t + half, tokens))
        count = jnp.maximum(jnp.minimum(t + half, tokens) - jnp.maximum(t - half, 0), 1)
        band = jnp.where(inside, 1.0 / count.astype(jnp.float32), 0.0) - (s == t).astype(jnp.float32)
        band = band.astype(jnp.bfloat16)
        squared = None
        for j in range(0, width, 256):
            branch = jnp.dot(band, normed[b - 16 : b - 16 + k, j : j + 256], preferred_element_type=jnp.float32)
            new = x_ref[b : b + m, j : j + 256].astype(jnp.float32) + branch * scale[:, j : j + 256]
            new = new.astype(jnp.bfloat16)
            if last:
                held[b - lo : b - lo + m, j : j + 256] = new
            else:
                out_ref[b : b + m, j : j + 256] = new
                new = new.astype(jnp.float32)
                new = new * new
                new = new[:, :128] + new[:, 128:]
                squared = new if squared is None else squared + new
        if last:
            rows = pl.ds(b - lo, m)
            copies.append(pltpu.make_async_copy(held.at[rows], out_ref.at[rows], sent.at[len(copies)]))
            copies[-1].start()
        else:
            acc[b : b + m] = squared
    if not last:
        sums_ref[...] = squares(acc[...])
    for copy in copies:
        copy.wait()


def over_tp(sums):
    n = lax.axis_size("tp")
    found = [sums]
    for k in (1, 3, 2):
        found.append(lax.ppermute(sums, "tp", [(i, i ^ k) for i in range(n)]))
    return found


def program(stream, norm_gain, pool_weight, pool_scale):
    rows, width = stream.shape
    layers, _, shard, _ = pool_weight.shape
    devices = lax.axis_size("sp")
    total = rows + 2 * HALO
    own = pool_weight.reshape(1, layers, shard, width)
    edge = jax.ShapeDtypeStruct((HALO, width), stream.dtype)
    fetched, within, across = pl.pallas_call(
        prepare_kernel,
        out_shape=(jax.ShapeDtypeStruct(own.shape, own.dtype), edge, edge),
        in_specs=[pl.BlockSpec(memory_space=pltpu.HBM)] * 2,
        out_specs=(VMEM,) * 3,
        scratch_shapes=[pltpu.VMEM((2, HALO, width), stream.dtype), pltpu.SemaphoreType.DMA((3,))],
        compiler_params=pltpu.CompilerParams(vmem_limit_bytes=123 * 2**19),
        name="prepare",
    )(own, stream)
    within = lax.ppermute(within, "sp", [(i, i ^ 1) for i in range(devices)])
    pairs = [(i, i + 1) for i in range(1, devices - 1, 2)]
    across = lax.ppermute(across, "sp", pairs + [(j, i) for i, j in pairs])
    params = pltpu.CompilerParams(vmem_limit_bytes=32 * 2**20)
    sums_type = jax.ShapeDtypeStruct((16, 128), jnp.float32)
    ext_type = jax.ShapeDtypeStruct((total, width), jnp.bfloat16)
    ext, sums = pl.pallas_call(
        first_kernel,
        out_shape=(ext_type, sums_type),
        in_specs=[VMEM, VMEM, pl.BlockSpec(memory_space=pltpu.HBM)],
        out_specs=(VMEM, VMEM),
        scratch_shapes=[pltpu.SemaphoreType.DMA((4,))],
        compiler_params=params,
        name="first",
    )(within, across, stream)
    other = lax.ppermute(sums, "tp", [(i, i ^ 1) for i in range(lax.axis_size("tp"))])
    gathered, early = gather(own, fetched)
    other = after(other, early)
    sums = pl.pallas_call(
        add_kernel, out_shape=sums_type, in_specs=[VMEM] * 2, out_specs=VMEM,
        compiler_params=pltpu.CompilerParams(vmem_limit_bytes=2**20), name="add",
    )(sums, other)
    other = lax.ppermute(sums, "tp", [(i, i ^ 3) for i in range(lax.axis_size("tp"))])
    traded = [sums, other]
    for layer in range(layers):
        pieces = finish(*gathered[layer], sums) if layer else gathered[0]
        last = layer == layers - 1
        lo, hi = (HALO, HALO + rows) if last else (16, total - 16)
        mapped = pl.pallas_call(
            functools.partial(map_kernel, layer, [p[1:] for p in pieces]),
            out_shape=jax.ShapeDtypeStruct((total, width), jnp.float32),
            in_specs=[VMEM] * (2 + len(pieces)),
            out_specs=VMEM,
            scratch_shapes=[pltpu.VMEM((width, width), jnp.bfloat16)],
            compiler_params=params,
            cost_estimate=pl.CostEstimate(
                flops=2 * total * width * width, bytes_accessed=6 * total * width, transcendentals=0
            ),
        )(ext, norm_gain, *[p[0] for p in pieces])
        scratch = [pltpu.VMEM((total, width), jnp.bfloat16)]
        if last:
            scratch += [pltpu.VMEM((rows, width), jnp.bfloat16), pltpu.SemaphoreType.DMA((5,))]
        else:
            scratch.append(pltpu.VMEM((total, 128), jnp.float32))
        out = pl.pallas_call(
            functools.partial(pool_kernel, layer, lo, hi, last, rows * devices, len(traded)),
            out_shape=jax.ShapeDtypeStruct((rows, width), jnp.bfloat16) if last else (ext_type, sums_type),
            in_specs=[VMEM] * (3 + len(traded)),
            out_specs=pl.BlockSpec(memory_space=pltpu.HBM) if last else (VMEM, VMEM),
            scratch_shapes=scratch,
            compiler_params=params,
            cost_estimate=pl.CostEstimate(
                flops=total * width * 512, bytes_accessed=8 * total * width, transcendentals=0
            ),
        )(ext, mapped, pool_scale, *traded)
        if not last:
            ext, sums = out
            traded = over_tp(sums)
    return out


def solution(mesh):
    placed = (P("sp", "tp"), P(None, "tp"), P(None, "tp", "sp", None), P(None, "tp"))
    return jax.shard_map(program, mesh=mesh, in_specs=placed, out_specs=P("sp", "tp"), check_vma=False)
```
